32 devices in a mesh: ep: 8 (over z, x), tp: 4 (over y, core).
Axes of the slice: x: 2, y: 2, z: 4, core: 2. Of those that a mesh axis runs over, the one named last changes fastest.
Arguments:
- tokens: bfloat16 [8192, 2048], P(('ep', 'tp')), may hold values from -6 to 6
- pre_gain: float32 [2048], replicated, may hold values from 0.1 to 1.9
- post_gain: float32 [2048], replicated, may hold values from 0.1 to 1.9
- expert_ids: int32 [8192, 2], P(('ep', 'tp')), may hold values from 0 to 7, as said below
- route_weight: float32 [8192, 2], P(('ep', 'tp')), may hold values from 0.1 to 1
- w_gate: bfloat16 [8, 2048, 512], P('ep', None, 'tp'), may hold values from -0.125 to 0.125
- w_up: bfloat16 [8, 2048, 512], P('ep', None, 'tp'), may hold values from -0.125 to 0.125
- w_down: bfloat16 [8, 2048, 512], P('ep', None, 'tp'), may hold values from -0.25 to 0.25
Outputs:
- layer_out: bfloat16 [8192, 2048], P(('ep', 'tp'))
The draws below stay inside these ranges and needn't reach their ends.
Inputs may be any that keep to these rules, and one draw needn't show every extreme that they name: `expert_ids`: each token names two different experts of one group, group g being experts 4 * g to 4 * g + 3. Among the rows of one device (aligned blocks of 256 rows) no expert is named more than 128 times, and in every block some expert is named exactly 128 times; one expert is named 128 times in every block.
All inputs are finite; a program needn't handle non-finite values.
Results may differ from the reference program's by a relative error of at most 0.0071.
Values may be sent and summed in bfloat16 or wider, within the bound.
A program may use at most 64 MiB of HBM per device.

```python
import math
import jax
import jax.numpy as jnp
from jax import lax

D = 2048
FF = 512
TOP = 2
GROUP = 4
TOK_DEV = 256
EXPERTS = 8
CAP = 128
TOKENS = 8192


def draw_expert_ids(key, part):
    blocks = TOKENS // TOK_DEV
    share = TOP * TOK_DEV // EXPERTS
    pairs = EXPERTS // (2 * GROUP)
    star = jax.random.randint(jax.random.fold_in(key, 11), (), 0, EXPERTS)
    star_group = star // GROUP
    star_pair = star_group // 2
    star_side = star_group % 2
    star_local = star % GROUP
    place = jnp.arange(2 * share * 2, dtype=jnp.int32)
    hot_three = 3 * share
    first_role = jnp.where(place < 2 * share, 0, jnp.where(place < hot_three, 1, jnp.where(place < hot_three + share // 2, 0, 2)))
    second_role = jnp.where(place < share, 1, jnp.where(place < 2 * share, 2, jnp.where(place < hot_three, 3, jnp.where(place < hot_three + share // 2, 1, 3))))
    is_hot = place < hot_three

    def one_block(block):
        block_key = jax.random.fold_in(key, block)
        hot_side = jax.random.randint(jax.random.fold_in(block_key, 1), (pairs,), 0, 2)
        hot_side = jnp.where(jnp.arange(pairs) == star_pair, star_side, hot_side)
        perm_keys = jax.random.split(jax.random.fold_in(block_key, 2), 2 * pairs)
        perms = jax.vmap(lambda sub: jax.random.permutation(sub, GROUP))(perm_keys).astype(jnp.int32)
        star_row = perms[star_group]
        where_star = jnp.argmax(star_row == star_local)
        star_row = star_row.at[where_star].set(star_row[0]).at[0].set(star_local)
        perms = perms.at[star_group].set(star_row)
        pair_index = jnp.arange(pairs, dtype=jnp.int32)[:, None]
        group = 2 * pair_index + jnp.where(is_hot[None, :], hot_side[:, None], 1 - hot_side[:, None])
        first = group * GROUP + perms[group, first_role[None, :]]
        second = group * GROUP + perms[group, second_role[None, :]]
        both = jnp.stack([first.reshape(-1), second.reshape(-1)], axis=1)
        shuffle = jax.random.permutation(jax.random.fold_in(block_key, 3), TOK_DEV)
        return both[shuffle]
    table = lax.map(one_block, jnp.arange(blocks, dtype=jnp.int32))
    return table.reshape(TOKENS, TOP).astype(jnp.int32)


def block_scale(rng, shape, shards, least, high):
    def one(dim, blocks):
        draws = jax.random.uniform(jax.random.fold_in(jax.random.fold_in(rng, 6), dim), (blocks,), jnp.float32, least / len(shards), high / len(shards))
        return jnp.repeat(jnp.exp(draws), shape[dim] // blocks).reshape((-1,) + (1,) * (len(shape) - dim - 1))

    level = one(*shards[0])
    for cut in shards[1:]:
        level = level * one(*cut)
    return level


def bell_draw(key, shape, spread, reach, cuts=(), kind=jnp.bfloat16):
    array = spread * jax.random.normal(key, shape, jnp.float32)
    if cuts:
        array = array * block_scale(key, shape, cuts, -0.22, 0.18)
    return jnp.clip(array, -reach, reach).astype(kind)


def setup_inputs(seed: int = 0) -> dict:
    streams_of = jax.random.split(jax.random.key(seed), 9)
    tokens = bell_draw(streams_of[0], (TOKENS, D), 1.0, 6.0, ((0, 32),))
    pre_gain = jnp.clip(1.0 + 0.18 * jax.random.normal(streams_of[1], (D,), jnp.float32), 0.1, 1.9)
    post_gain = jnp.clip(1.0 + 0.18 * jax.random.normal(streams_of[2], (D,), jnp.float32), 0.1, 1.9)
    expert_ids = draw_expert_ids(jax.random.fold_in(streams_of[8], 71), 0)
    route_weight = jnp.clip(jnp.exp(math.log(1.0) - 2.3025851 * jax.random.uniform(streams_of[4], (TOKENS, TOP), jnp.float32) ** block_scale(streams_of[4], (TOKENS, TOP), ((0, 32),), -0.2, 0.2)), 0.1, 1.0)
    w_gate = bell_draw(streams_of[5], (EXPERTS, D, FF), D ** -0.5, 0.125, ((0, 8), (2, 4)))
    w_up = bell_draw(streams_of[6], (EXPERTS, D, FF), D ** -0.5, 0.125, ((0, 8), (2, 4)))
    w_down = bell_draw(streams_of[7], (EXPERTS, D, FF), FF ** -0.5, 0.25, ((0, 8), (2, 4)))
    return dict(tokens=tokens, pre_gain=pre_gain, post_gain=post_gain, expert_ids=expert_ids, route_weight=route_weight, w_gate=w_gate, w_up=w_up, w_down=w_down)


def rms_scale(values, gain):
    mean_sq = lax.optimization_barrier(jnp.mean(values * values, axis=-1, keepdims=True))
    return values * lax.rsqrt(mean_sq + 1e-06) * gain

def reference(tokens, pre_gain, post_gain, expert_ids, route_weight, w_gate, w_up, w_down):
    count = tokens.shape[0]
    width = tokens.shape[1]
    normed = rms_scale(tokens.astype(jnp.float32), pre_gain).astype(jnp.bfloat16)
    padded = jnp.concatenate([normed, jnp.zeros((1, width), jnp.bfloat16)], axis=0)
    flat = expert_ids.reshape(-1).astype(jnp.int32)
    routes = flat.shape[0]
    order = jnp.argsort(flat, stable=True).astype(jnp.int32)
    sorted_ids = flat[order]
    first = jnp.searchsorted(sorted_ids, sorted_ids, side='left').astype(jnp.int32)
    rank = jnp.arange(routes, dtype=jnp.int32) - first
    global_cap = count // TOK_DEV * CAP
    table = jnp.full((EXPERTS * global_cap,), routes, jnp.int32)
    table = table.at[sorted_ids * global_cap + rank].set(order).reshape(EXPERTS, global_cap)

    def one_expert(index):
        slots = table[index]
        rows = padded[jnp.minimum(slots // TOP, count).astype(jnp.int32)]
        rows = jnp.where((slots < routes)[:, None], rows, jnp.zeros_like(rows))
        gate = jnp.dot(rows, w_gate[index], preferred_element_type=jnp.float32)
        up = jnp.dot(rows, w_up[index], preferred_element_type=jnp.float32)
        hidden = (jax.nn.silu(gate) * up).astype(jnp.bfloat16)
        return jnp.dot(hidden, w_down[index].T, preferred_element_type=jnp.float32).astype(jnp.bfloat16)
    results = lax.map(one_expert, jnp.arange(EXPERTS, dtype=jnp.int32))
    per_route = jnp.zeros((routes + 1, width), jnp.bfloat16)
    per_route = per_route.at[table.reshape(-1)].set(results.reshape(-1, width))
    per_route = per_route[:routes].reshape(count, TOP, width)
    mixed = lax.optimization_barrier(jnp.sum(per_route.astype(jnp.float32) * route_weight[:, :, None], axis=1))
    return rms_scale(mixed, post_gain).astype(jnp.bfloat16)
```

```python
import functools

import jax
import jax.numpy as jnp
from jax import lax
from jax.experimental import pallas as pl
from jax.experimental.pallas import tpu as pltpu
from jax.sharding import PartitionSpec as P


def rms_scale(values, gain):
    mean_sq = jnp.mean(values * values, axis=-1, keepdims=True)
    return values * lax.rsqrt(mean_sq + 1e-06) * gain


def expert_terms(rows, gate_part, up_part, down_part):
    gate = jnp.dot(rows, gate_part, preferred_element_type=jnp.float32)
    up = jnp.dot(rows, up_part, preferred_element_type=jnp.float32)
    hidden = (jax.nn.silu(gate) * up).astype(jnp.bfloat16)
    return lax.dot_general(
        hidden, down_part, (((1,), (1,)), ((), ())), preferred_element_type=jnp.float32
    )


def collect_expert(w_gate, w_up, w_down):
    return (
        lax.all_gather(w_gate, "tp", axis=2, tiled=True),
        lax.all_gather(w_up, "tp", axis=2, tiled=True),
        lax.all_gather(w_down, "tp", axis=2, tiled=True),
    )


def body(tokens, pre_gain, post_gain, expert_ids, route_weight, w_gate, w_up, w_down):
    count, width = tokens.shape
    top = expert_ids.shape[1]
    experts = lax.axis_size("ep") * w_gate.shape[0]
    capacity = 2 * top * count // experts
    normed = rms_scale(tokens.astype(jnp.float32), pre_gain).astype(jnp.bfloat16)
    flat = expert_ids.reshape(-1)
    onehot = (flat[:, None] == jnp.arange(experts, dtype=jnp.int32)[None, :]).astype(jnp.int32)
    rank = jnp.sum((jnp.cumsum(onehot, axis=0) - onehot) * onehot, axis=1)
    target = flat * capacity + rank
    source = jnp.full((experts * capacity,), count, jnp.int32)
    source = source.at[target].set(jnp.arange(count * top, dtype=jnp.int32) // top)
    padded = jnp.concatenate([normed, jnp.zeros((1, width), jnp.bfloat16)], axis=0)
    outgoing = padded[source].reshape(experts, capacity, width)
    arrived = lax.all_to_all(outgoing, "ep", split_axis=0, concat_axis=0, tiled=True)
    rows = arrived.reshape(experts * capacity, width)
    gate_all, up_all, down_all = collect_expert(w_gate, w_up, w_down)
    result = expert_terms(rows, gate_all[0], up_all[0], down_all[0])
    answer = result.astype(jnp.bfloat16).reshape(experts, capacity, width)
    returned = lax.all_to_all(answer, "ep", split_axis=0, concat_axis=0, tiled=True)
    per_route = returned.reshape(experts * capacity, width)[target].reshape(count, top, width)
    mixed = jnp.sum(per_route.astype(jnp.float32) * route_weight[:, :, None], axis=1)
    return rms_scale(mixed, post_gain).astype(jnp.bfloat16)

MESH = pl.DeviceIdType.MESH
CUTS = 8
NEAR_CUTS = 4
LAG = 3
AHEAD = 4
Z_FIRST = (0, 4)
PLACE = (0, 3, 1, 2)
VMEM_BYTES = 60 * 2**20


def flip(index, stride):
    return index + stride - 2 * stride * lax.rem(lax.div(index, stride), 2)


def kernel(
    n_ep, tok, pre, post, ids, rw, wg, wu, wd, out,
    T, XT, XC, IDS, RW, PRE, POST, WR, RK, COL, GU, DN, H, HX, EC, SN, SF, RN, RF, ZS, ZR, ACC,
    loc, t_send, t1_recv, t_recv, w_send, w_recv, g_send, g_recv, g2_recv, gf_recv, d_send, d_recv, df_recv,
    s_send, n_recv, m_recv, f_recv, z_recv,
):
    count, width = tok.shape
    part = wg.shape[2]
    experts = WR.shape[1]
    cap = EC.shape[2]
    half = n_ep // 2
    bf, f32 = jnp.bfloat16, jnp.float32
    e, t = lax.axis_index("ep"), lax.axis_index("tp")
    to_x, to_z, to_h = (flip(e, 1), t), (flip(e, 2), t), (flip(e, half), t)
    to_c, to_y = (e, flip(t, 1)), (e, flip(t, 2))

    barrier = pltpu.get_barrier_semaphore()
    for who in (to_x, to_z, to_h, to_c, to_y):
        pl.semaphore_signal(barrier, inc=1, device_id=who, device_id_type=MESH)

    own = [
        pltpu.make_async_copy(ids, IDS, loc.at[0]),
        pltpu.make_async_copy(rw, RW, loc.at[1]),
        pltpu.make_async_copy(tok, T.at[0], loc.at[2]),
        pltpu.make_async_copy(wg.at[0], GU.at[0, :, pl.ds(0, part)], loc.at[3]),
        pltpu.make_async_copy(wu.at[0], GU.at[0, :, pl.ds(part, part)], loc.at[4]),
        pltpu.make_async_copy(wd.at[0], DN.at[:, pl.ds(0, part)], loc.at[5]),
        pltpu.make_async_copy(pre, PRE, loc.at[6]),
        pltpu.make_async_copy(post, POST, loc.at[7]),
    ]
    for copy in own:
        copy.start()

    def remote(src, dst, send, recv, who):
        return pltpu.make_async_remote_copy(
            src_ref=src, dst_ref=dst, send_sem=send, recv_sem=recv, device_id=who, device_id_type=MESH
        )

    def rows_of(total, cuts, j):
        return pl.ds(0, total) if j is None else pl.ds(j * (total // cuts), total // cuts)

    block_from = {1: (0, to_z), 2: (0, to_x), 3: (1, to_x)}

    def routes(k):
        s, who = block_from[k]
        return remote(WR.at[s], WR.at[k], w_send.at[k - 1], w_recv.at[k - 1], who)

    def tokens(k, j=None):
        s, who = block_from[k]
        rows = rows_of(count, CUTS, j)
        recv = t1_recv.at[j] if k == 1 and j is not None else t_recv.at[k - 1]
        return remote(T.at[s, rows], T.at[k, rows], t_send.at[k - 1], recv, who)

    def route(k):
        if k % 2:
            return k - 1, to_c
        if k % 4:
            return k - 2, to_y
        return 0, to_h

    def gu(k, j=None):
        s, who = route(k)
        rows = rows_of(width, NEAR_CUTS if k in (2, 3) else CUTS, j)
        recv = g_recv.at[k - 1]
        if j is not None and k == 2:
            recv = g2_recv.at[j]
        if j is not None and k in (4, 6):
            recv = gf_recv.at[k // 2 - 2, j]
        return remote(GU.at[s, rows], GU.at[k, rows], g_send.at[k - 1], recv, who)

    def dn(k, j=None):
        s, who = route(k)
        rows = rows_of(width, CUTS, j)
        recv = d_recv.at[k - 1] if k < 4 else df_recv.at[k - 4, 0 if j is None else j]
        return remote(
            DN.at[rows, pl.ds(s * part, part)], DN.at[rows, pl.ds(k * part, part)], d_send.at[k - 1], recv, who
        )

    cols = width // CUTS

    def lane_block(j):
        return pl.ds(j * cols, cols)

    def first(kind, j, rows=None):
        src, dst = (SN, RN) if kind < 2 else (SF, RF)
        rows = pl.ds(0, 2 * cap) if rows is None else rows
        recv = (n_recv, m_recv, f_recv)[kind].at[j]
        return remote(src.at[j, rows], dst.at[j, rows], s_send.at[kind // 2], recv, to_z if j in Z_FIRST else to_x)

    def second(j):
        return remote(ZS.at[j], ZR.at[j], s_send.at[2], z_recv.at[j], to_x if j in Z_FIRST else to_z)

    which = lax.broadcasted_iota(jnp.int32, (experts, count), 0)
    mine = (e, lax.rem(e + half, n_ep))
    of_x = (flip(e, 1), lax.rem(flip(e, 1) + half, n_ep))
    of_z = (flip(e, 2), lax.rem(flip(e, 2) + half, n_ep))

    def row_of(table, expert):
        return jnp.sum(jnp.where(which == expert, table, 0.0), axis=0, keepdims=True)

    def own_routes():
        picks = [jnp.where(IDS[k : k + 1, :] == which, RW[k : k + 1, :], 0.0) for k in range(ids.shape[0])]
        total = picks[0]
        for pick in picks[1:]:
            total = total + pick
        WR[0] = total

    def ranks(block):
        named = WR[block] > 0.0
        ones = jnp.where(named, 1.0, 0.0)
        before = lax.broadcasted_iota(jnp.int32, (count, count), 0) <= lax.broadcasted_iota(
            jnp.int32, (count, count), 1
        )
        upto = jnp.dot(ones, jnp.where(before, 1.0, 0.0), preferred_element_type=f32)
        RK[block] = jnp.where(named, upto - 1.0, -1.0)

    def norm(block, slot, low, high):
        def some(i, carry):
            rows = pl.ds(pl.multiple_of(i * 16, 16), 16)
            values = T[block, rows, :].astype(f32)
            XT[slot, rows, :] = rms_scale(values, PRE[...]).astype(bf)
            return carry

        lax.fori_loop(low // 16, high // 16, some, 0)

    def gather(block, slot):
        rows = pl.ds(PLACE[block] * cap, cap)
        for h in range(2):
            at = row_of(RK[block], mine[h])
            hit = lax.broadcasted_iota(jnp.int32, (cap, count), 0).astype(f32) == at
            weight = jnp.sum(jnp.where(hit, row_of(WR[block], mine[h]), 0.0), axis=1, keepdims=True)
            COL[h, rows, :] = jnp.broadcast_to(weight, (cap, part))
            pick = jnp.where(hit, 1.0, 0.0).astype(bf)

            def tile(i, carry):
                lanes = pl.ds(pl.multiple_of(i * 256, 256), 256)
                XC[h, rows, lanes] = jnp.dot(pick, XT[slot, :, lanes], preferred_element_type=f32).astype(bf)
                return carry

            lax.fori_loop(0, width // 256, tile, 0)

    def spread(block, base, whose):
        eye = lax.broadcasted_iota(jnp.int32, (count, count), 0) == lax.broadcasted_iota(
            jnp.int32, (count, count), 1
        )
        for h in range(2):
            at = jnp.sum(jnp.where(eye, row_of(RK[block], whose[h]), 0.0), axis=1, keepdims=True)
            hit = lax.broadcasted_iota(jnp.int32, (count, cap), 1).astype(f32) == at
            EC[base + h] = jnp.where(hit, 1.0, 0.0).astype(bf)

    def hidden(low, high, a, b):
        h = low // 4
        rows = pl.ds(a * cap, (b - a) * cap)

        def one(s, carry):
            both = jnp.dot(XC[h, rows, :], GU[s], preferred_element_type=f32)
            gate, up = both[:, :part], both[:, part:]
            value = gate / (1.0 + jnp.exp(-gate)) * up * COL[h, rows, :]
            H[h, rows, pl.ds(pl.multiple_of((s - 4 * h) * part, part), part)] = value.astype(bf)
            return carry

        lax.fori_loop(low, high, one, 0)

    def times(left, right):
        return lax.dot_general(left, right, (((1,), (1,)), ((), ())), preferred_element_type=f32)

    def down(h, place, n, j):
        left = H[h, pl.ds(place * cap, n * cap), :]
        return times(left, DN[lane_block(j), pl.ds(h * 4 * part, 4 * part)]).astype(bf)

    def widen(block, base, halves):
        for h in halves:
            left = jnp.dot(EC[base + h], H[h, pl.ds(PLACE[block] * cap, cap), :], preferred_element_type=f32)
            HX[block, :, pl.ds(h * 4 * part, 4 * part)] = left.astype(bf)

    def total(block, base, at, j):
        rows = pl.ds(at * cap, cap)
        return (
            times(HX[block], DN[lane_block(j), :])
            + jnp.dot(EC[base], RN[j, rows, :], preferred_element_type=f32)
            + jnp.dot(EC[base + 1], RF[j, rows, :], preferred_element_type=f32)
        )

    for copy in own[:2]:
        copy.wait()
    own_routes()
    own[2].wait()
    pl.semaphore_wait(barrier, 5)
    for k in (1, 2):
        routes(k).start()
    for copy in own[3:5]:
        copy.wait()
    for j in range(CUTS):
        tokens(1, j).start()
        gu(4, j).start()
        if j == 0:
            tokens(2).start()
            gu(1).start()
        if j % (CUTS // NEAR_CUTS) == 0:
            gu(2, j * NEAR_CUTS // CUTS).start()
    own[5].wait()
    dn(1).start()
    dn(2).start()
    for j in range(AHEAD):
        dn(4, j).start()
    for copy in own[6:]:
        copy.wait()
    ranks(0)
    norm(0, 0, 0, count)
    gather(0, 0)
    spread(0, 0, mine)
    routes(1).wait_recv()
    routes(3).start()
    ranks(1)
    routes(2).wait_recv()
    ranks(2)
    spread(0, 2, of_x)

    def far(j):
        gu(4, j).wait_recv()
        gu(6, j).start()
        gu(5, j).start()

    def far_mate(j):
        gu(6, j).wait_recv()
        gu(7, j).start()

    def down_far(j):
        dn(4, j).wait_recv()
        if j + AHEAD < CUTS:
            dn(4, j + AHEAD).start()
        dn(6, j).start()
        dn(5, j).start()

    def down_mate(j):
        dn(6, j).wait_recv()
        dn(7, j).start()

    t_rows = count // CUTS
    for i in range(CUTS):
        tokens(1, i).wait_recv()
        tokens(3, i).start()
        far(i)
        if i < NEAR_CUTS:
            gu(2, i).wait_recv()
            gu(3, i).start()
        norm(1, 1, i * t_rows, (i + 1) * t_rows)
        if i == 0:
            spread(0, 4, of_z)
            spread(1, 6, mine)
        if i == 1:
            spread(1, 8, of_x)
            spread(2, 10, mine)
        if i == 2:
            spread(2, 12, of_z)
            routes(3).wait_recv()
            ranks(3)
        if i == NEAR_CUTS:
            tokens(2).wait_recv()
            norm(2, 0, 0, count)
            gather(2, 0)
            gu(1).wait_recv()
            gu(3).wait_recv()
            hidden(0, 4, 0, 2)
        if i == NEAR_CUTS + 1:
            dn(2).wait_recv()
            dn(3).start()
            far_mate(0)
        if i == NEAR_CUTS + 2:
            far_mate(1)
            dn(1).wait_recv()
            dn(3).wait_recv()
            for j in range(CUTS):
                if j not in Z_FIRST:
                    SN[j, :cap] = down(0, 1, 1, j)
                    first(0, j, pl.ds(0, cap)).start()
            far_mate(2)
    far_mate(3)
    gather(1, 1)
    tokens(3).wait_recv()
    norm(3, 0, 0, count)
    gather(3, 0)
    far_mate(4)
    hidden(0, 4, 2, 4)
    for j in range(CUTS):
        if j in Z_FIRST:
            SN[j] = down(0, 2, 2, j)
            first(1, j).start()
        else:
            SN[j, cap:] = down(0, 2, 1, j)
            first(1, j, pl.ds(cap, cap)).start()
    far_mate(5)
    down_far(0)
    widen(0, 0, (0,))
    widen(1, 6, (0,))
    widen(2, 10, (0,))
    gu(5).wait_recv()
    far_mate(6)
    hidden(4, 6, 0, 4)
    down_far(1)
    far_mate(7)
    down_far(2)
    gu(7).wait_recv()
    hidden(6, 8, 0, 4)
    down_mate(0)
    down_far(3)

    def pass_on(j):
        first(2, j).wait_recv()
        if j in Z_FIRST:
            first(1, j).wait_recv()
            kept, base, home, from_home, at = 2, 12, 4, 1, 0
        else:
            first(0, j, pl.ds(0, cap)).wait_recv()
            first(1, j, pl.ds(cap, cap)).wait_recv()
            kept, base, home, from_home, at = 1, 8, 2, 0, 1
        ZS[j] = total(kept, base, at, j).astype(bf)
        second(j).start()
        ACC[j] = total(0, home, from_home, j)

    for j in range(CUTS):
        if j + 4 < CUTS:
            down_far(j + 4)
        if j + 1 < CUTS:
            down_mate(j + 1)
        dn(5, j).wait_recv()
        dn(7, j).wait_recv()
        SF[j] = down(1, 2 if j in Z_FIRST else 1, 2, j)
        first(2, j).start()
        if j == 0:
            widen(0, 0, (1,))
            widen(1, 6, (1,))
            widen(2, 10, (1,))
        if j >= LAG:
            pass_on(j - LAG)
    for j in range(CUTS - LAG, CUTS):
        pass_on(j)
    square = jnp.zeros((count, 1), f32)
    for j in range(CUTS):
        second(j).wait_recv()
        mixed = ACC[j] + ZR[j].astype(f32)
        ACC[j] = mixed
        square = square + jnp.sum(mixed * mixed, axis=1, keepdims=True)
    scale = lax.rsqrt(square / width + 1e-06)
    for j in range(CUTS):
        out[:, lane_block(j)] = (ACC[j] * scale * POST[:, lane_block(j)]).astype(bf)
    for k in (1, 2, 3):
        routes(k).wait_send()
        tokens(k).wait_send()
    for k in range(1, 8):
        gu(k).wait_send()
        dn(k).wait_send()
    for kind, (src, dst) in enumerate(((SN, RN), (SF, RF), (ZS, ZR))):
        remote(src, dst, s_send.at[kind], z_recv.at[0], to_x).wait_send()


def fused(n_ep, tokens, pre_gain, post_gain, expert_ids, route_weight, w_gate, w_up, w_down):
    count, width = tokens.shape
    top = expert_ids.shape[1]
    part = w_gate.shape[2]
    experts = n_ep * w_gate.shape[0]
    cap = 2 * top * count // experts
    bf, f32 = jnp.bfloat16, jnp.float32
    cols = width // CUTS
    anywhere = pl.BlockSpec(memory_space=pl.ANY)
    vmem = pl.BlockSpec(memory_space=pltpu.VMEM)
    dma = pltpu.SemaphoreType.DMA
    return pl.pallas_call(
        functools.partial(kernel, n_ep),
        out_shape=jax.ShapeDtypeStruct((count, width), bf),
        in_specs=[anywhere] * 8,
        out_specs=vmem,
        scratch_shapes=[
            pltpu.VMEM((4, count, width), bf),
            pltpu.VMEM((2, count, width), bf),
            pltpu.VMEM((2, 4 * cap, width), bf),
            pltpu.VMEM((top, count), jnp.int32),
            pltpu.VMEM((top, count), f32),
            pltpu.VMEM((1, width), f32),
            pltpu.VMEM((1, width), f32),
            pltpu.VMEM((4, experts, count), f32),
            pltpu.VMEM((4, experts, count), f32),
            pltpu.VMEM((2, 4 * cap, part), f32),
            pltpu.VMEM((8, width, 2 * part), bf),
            pltpu.VMEM((width, 8 * part), bf),
            pltpu.VMEM((2, 4 * cap, 4 * part), bf),
            pltpu.VMEM((3, count, 8 * part), bf),
            pltpu.VMEM((14, count, cap), bf),
            pltpu.VMEM((CUTS, 2 * cap, cols), bf),
            pltpu.VMEM((CUTS, 2 * cap, cols), bf),
            pltpu.VMEM((CUTS, 2 * cap, cols), bf),
            pltpu.VMEM((CUTS, 2 * cap, cols), bf),
            pltpu.VMEM((CUTS, count, cols), bf),
            pltpu.VMEM((CUTS, count, cols), bf),
            pltpu.VMEM((CUTS, count, cols), f32),
            dma((8,)),
            dma((3,)), dma((CUTS,)), dma((3,)), dma((3,)), dma((3,)),
            dma((7,)), dma((7,)), dma((NEAR_CUTS,)), dma((2, CUTS)),
            dma((7,)), dma((3,)), dma((4, CUTS)),
            dma((3,)), dma((CUTS,)), dma((CUTS,)), dma((CUTS,)), dma((CUTS,)),
        ],
        compiler_params=pltpu.CompilerParams(
            collective_id=0, has_side_effects=True, vmem_limit_bytes=VMEM_BYTES
        ),
    )(tokens, pre_gain[None], post_gain[None], expert_ids.T, route_weight.T, w_gate, w_up, w_down)


def whole_body(n_ep, n_tp, *args):
    lanes = args[5].shape[2]
    if n_ep // 2 == n_tp == 2 * 2 and args[5].shape[0] == 1 and lanes % 128 == 0:
        return fused(n_ep, *args)
    return body(*args)


def solution(mesh):
    in_specs = (
        P(("ep", "tp"), None),
        P(),
        P(),
        P(("ep", "tp"), None),
        P(("ep", "tp"), None),
        P("ep", None, "tp"),
        P("ep", None, "tp"),
        P("ep", None, "tp"),
    )
    out_specs = P(("ep", "tp"), None)
    step = functools.partial(whole_body, mesh.shape["ep"], mesh.shape["tp"])
    return jax.shard_map(step, mesh=mesh, in_specs=in_specs, out_specs=out_specs, check_vma=False)
```

```python
import functools

import jax
import jax.numpy as jnp
from jax import lax
from jax.experimental import pallas as pl
from jax.experimental.pallas import tpu as pltpu
from jax.sharding import PartitionSpec as P


def rms_scale(values, gain):
    mean_sq = jnp.mean(values * values, axis=-1, keepdims=True)
    return values * lax.rsqrt(mean_sq + 1e-06) * gain


def expert_terms(rows, gate_part, up_part, down_part):
    gate = jnp.dot(rows, gate_part, preferred_element_type=jnp.float32)
    up = jnp.dot(rows, up_part, preferred_element_type=jnp.float32)
    hidden = (jax.nn.silu(gate) * up).astype(jnp.bfloat16)
    return lax.dot_general(
        hidden, down_part, (((1,), (1,)), ((), ())), preferred_element_type=jnp.float32
    )


def collect_expert(w_gate, w_up, w_down):
    return (
        lax.all_gather(w_gate, "tp", axis=2, tiled=True),
        lax.all_gather(w_up, "tp", axis=2, tiled=True),
        lax.all_gather(w_down, "tp", axis=2, tiled=True),
    )


def body(tokens, pre_gain, post_gain, expert_ids, route_weight, w_gate, w_up, w_down):
    count, width = tokens.shape
    top = expert_ids.shape[1]
    experts = lax.axis_size("ep") * w_gate.shape[0]
    capacity = 2 * top * count // experts
    normed = rms_scale(tokens.astype(jnp.float32), pre_gain).astype(jnp.bfloat16)
    flat = expert_ids.reshape(-1)
    onehot = (flat[:, None] == jnp.arange(experts, dtype=jnp.int32)[None, :]).astype(jnp.int32)
    rank = jnp.sum((jnp.cumsum(onehot, axis=0) - onehot) * onehot, axis=1)
    target = flat * capacity + rank
    source = jnp.full((experts * capacity,), count, jnp.int32)
    source = source.at[target].set(jnp.arange(count * top, dtype=jnp.int32) // top)
    padded = jnp.concatenate([normed, jnp.zeros((1, width), jnp.bfloat16)], axis=0)
    outgoing = padded[source].reshape(experts, capacity, width)
    arrived = lax.all_to_all(outgoing, "ep", split_axis=0, concat_axis=0, tiled=True)
    rows = arrived.reshape(experts * capacity, width)
    gate_all, up_all, down_all = collect_expert(w_gate, w_up, w_down)
    result = expert_terms(rows, gate_all[0], up_all[0], down_all[0])
    answer = result.astype(jnp.bfloat16).reshape(experts, capacity, width)
    returned = lax.all_to_all(answer, "ep", split_axis=0, concat_axis=0, tiled=True)
    per_route = returned.reshape(experts * capacity, width)[target].reshape(count, top, width)
    mixed = jnp.sum(per_route.astype(jnp.float32) * route_weight[:, :, None], axis=1)
    return rms_scale(mixed, post_gain).astype(jnp.bfloat16)

MESH = pl.DeviceIdType.MESH
CUTS = 8
NEAR_CUTS = 4
LAG = 3
AHEAD = 4
Z_FIRST = (2, 5)
PLACE = (0, 3, 1, 2)
VMEM_BYTES = 60 * 2**20


def flip(index, stride):
    return index + stride - 2 * stride * lax.rem(lax.div(index, stride), 2)


def kernel(
    n_ep, tok, pre, post, ids, rw, wg, wu, wd, out,
    T, X, XC, IDS, RW, PRE, POST, WR, RK, COL, GU, DN, H, HX, EC, SN, SF, RN, RF, ZS, ZR, ACC,
    loc, t_send, t1_recv, t_recv, w_send, w_recv, g_send, g_recv, g2_recv, gf_recv, d_send, d_recv, df_recv,
    s_send, n_recv, m_recv, f_recv, z_recv,
):
    count, width = tok.shape
    part = wg.shape[2]
    experts = WR.shape[1]
    cap = EC.shape[2]
    half = n_ep // 2
    bf, f32 = jnp.bfloat16, jnp.float32
    e, t = lax.axis_index("ep"), lax.axis_index("tp")
    to_x, to_z, to_h = (flip(e, 1), t), (flip(e, 2), t), (flip(e, half), t)
    to_c, to_y = (e, flip(t, 1)), (e, flip(t, 2))

    barrier = pltpu.get_barrier_semaphore()
    for who in (to_x, to_z, to_h, to_c, to_y):
        pl.semaphore_signal(barrier, inc=1, device_id=who, device_id_type=MESH)

    own = [
        pltpu.make_async_copy(ids, IDS, loc.at[0]),
        pltpu.make_async_copy(rw, RW, loc.at[1]),
        pltpu.make_async_copy(tok, T, loc.at[2]),
        pltpu.make_async_copy(wg.at[0], GU.at[0, :, pl.ds(0, part)], loc.at[3]),
        pltpu.make_async_copy(wu.at[0], GU.at[0, :, pl.ds(part, part)], loc.at[4]),
        pltpu.make_async_copy(wd.at[0], DN.at[:, pl.ds(0, part)], loc.at[5]),
        pltpu.make_async_copy(pre, PRE, loc.at[6]),
        pltpu.make_async_copy(post, POST, loc.at[7]),
    ]
    for copy in own:
        copy.start()

    def remote(src, dst, send, recv, who):
        return pltpu.make_async_remote_copy(
            src_ref=src, dst_ref=dst, send_sem=send, recv_sem=recv, device_id=who, device_id_type=MESH
        )

    def rows_of(total, cuts, j):
        return pl.ds(0, total) if j is None else pl.ds(j * (total // cuts), total // cuts)

    block_from = {1: (0, to_z), 2: (0, to_x), 3: (1, to_x)}

    def routes(k):
        s, who = block_from[k]
        return remote(WR.at[s], WR.at[k], w_send.at[k - 1], w_recv.at[k - 1], who)

    def tokens(k, j=None):
        s, who = block_from[k]
        rows = rows_of(count, CUTS, j)
        recv = t1_recv.at[j] if k == 1 and j is not None else t_recv.at[k - 1]
        return remote(X.at[s, rows], X.at[k, rows], t_send.at[k - 1], recv, who)

    def route(k):
        if k % 2:
            return k - 1, to_c
        if k % 4:
            return k - 2, to_y
        return 0, to_h

    def gu(k, j=None):
        s, who = route(k)
        rows = rows_of(width, NEAR_CUTS if k in (2, 3) else CUTS, j)
        recv = g_recv.at[k - 1]
        if j is not None and k == 2:
            recv = g2_recv.at[j]
        if j is not None and k in (4, 6):
            recv = gf_recv.at[k // 2 - 2, j]
        return remote(GU.at[s, rows], GU.at[k, rows], g_send.at[k - 1], recv, who)

    def dn(k, j=None):
        s, who = route(k)
        rows = rows_of(width, CUTS, j)
        recv = d_recv.at[k - 1] if k < 4 else df_recv.at[k - 4, 0 if j is None else j]
        return remote(
            DN.at[rows, pl.ds(s * part, part)], DN.at[rows, pl.ds(k * part, part)], d_send.at[k - 1], recv, who
        )

    cols = width // CUTS

    def lane_block(j):
        return pl.ds(j * cols, cols)

    def first(kind, j, rows=None):
        src, dst = (SN, RN) if kind < 2 else (SF, RF)
        rows = pl.ds(0, 2 * cap) if rows is None else rows
        recv = (n_recv, m_recv, f_recv)[kind].at[j]
        return remote(src.at[j, rows], dst.at[j, rows], s_send.at[kind // 2], recv, to_z if j in Z_FIRST else to_x)

    def second(j):
        return remote(ZS.at[j], ZR.at[j], s_send.at[2], z_recv.at[j], to_x if j in Z_FIRST else to_z)

    which = lax.broadcasted_iota(jnp.int32, (experts, count), 0)
    mine = (e, lax.rem(e + half, n_ep))
    of_x = (flip(e, 1), lax.rem(flip(e, 1) + half, n_ep))
    of_z = (flip(e, 2), lax.rem(flip(e, 2) + half, n_ep))

    def row_of(table, expert):
        return jnp.sum(jnp.where(which == expert, table, 0.0), axis=0, keepdims=True)

    def own_routes():
        picks = [jnp.where(IDS[k : k + 1, :] == which, RW[k : k + 1, :], 0.0) for k in range(ids.shape[0])]
        total = picks[0]
        for pick in picks[1:]:
            total = total + pick
        WR[0] = total

    def ranks(block):
        named = WR[block] > 0.0
        ones = jnp.where(named, 1.0, 0.0)
        before = lax.broadcasted_iota(jnp.int32, (count, count), 0) <= lax.broadcasted_iota(
            jnp.int32, (count, count), 1
        )
        upto = jnp.dot(ones, jnp.where(before, 1.0, 0.0), preferred_element_type=f32)
        RK[block] = jnp.where(named, upto - 1.0, -1.0)

    def norm():
        def some(i, carry):
            rows = pl.ds(pl.multiple_of(i * 16, 16), 16)
            X[0, rows, :] = rms_scale(T[rows, :].astype(f32), PRE[...]).astype(bf)
            return carry

        lax.fori_loop(0, count // 16, some, 0, unroll=4)

    def gather(block):
        rows = pl.ds(PLACE[block] * cap, cap)
        picks = []
        for h in range(2):
            at = row_of(RK[block], mine[h])
            hit = lax.broadcasted_iota(jnp.int32, (cap, count), 0).astype(f32) == at
            weight = jnp.sum(jnp.where(hit, row_of(WR[block], mine[h]), 0.0), axis=1, keepdims=True)
            COL[h, rows, :] = jnp.broadcast_to(weight, (cap, part))
            picks.append(jnp.where(hit, 1.0, 0.0).astype(bf))
        pick = jnp.concatenate(picks, axis=0)
        step = width // 4
        for i in range(4):
            lanes = pl.ds(i * step, step)
            found = jnp.dot(pick, X[block, :, lanes], preferred_element_type=f32).astype(bf)
            XC[0, rows, lanes] = found[:cap]
            XC[1, rows, lanes] = found[cap:]

    def spread(block, base, whose):
        eye = lax.broadcasted_iota(jnp.int32, (count, count), 0) == lax.broadcasted_iota(
            jnp.int32, (count, count), 1
        )
        for h in range(2):
            at = jnp.sum(jnp.where(eye, row_of(RK[block], whose[h]), 0.0), axis=1, keepdims=True)
            hit = lax.broadcasted_iota(jnp.int32, (count, cap), 1).astype(f32) == at
            EC[base + h] = jnp.where(hit, 1.0, 0.0).astype(bf)

    def hidden(low, high, a, b):
        h = low // 4
        rows = pl.ds(a * cap, (b - a) * cap)

        def one(s, carry):
            both = jnp.dot(XC[h, rows, :], GU[s], preferred_element_type=f32)
            gate, up = both[:, :part], both[:, part:]
            value = gate / (1.0 + jnp.exp(-gate)) * up * COL[h, rows, :]
            H[h, rows, pl.ds(pl.multiple_of((s - 4 * h) * part, part), part)] = value.astype(bf)
            return carry

        lax.fori_loop(low, high, one, 0)

    def times(left, right):
        return lax.dot_general(left, right, (((1,), (1,)), ((), ())), preferred_element_type=f32)

    def down(h, place, n, j):
        left = H[h, pl.ds(place * cap, n * cap), :]
        return times(left, DN[lane_block(j), pl.ds(h * 4 * part, 4 * part)]).astype(bf)

    def widen(block, base, halves):
        for h in halves:
            left = jnp.dot(EC[base + h], H[h, pl.ds(PLACE[block] * cap, cap), :], preferred_element_type=f32)
            HX[block, :, pl.ds(h * 4 * part, 4 * part)] = left.astype(bf)

    def total(block, base, at, j):
        rows = pl.ds(at * cap, cap)
        return (
            times(HX[block], DN[lane_block(j), :])
            + jnp.dot(EC[base], RN[j, rows, :], preferred_element_type=f32)
            + jnp.dot(EC[base + 1], RF[j, rows, :], preferred_element_type=f32)
        )

    for copy in own[:2]:
        copy.wait()
    own_routes()
    own[2].wait()
    own[6].wait()
    norm()
    pl.semaphore_wait(barrier, 5)
    for k in (1, 2):
        routes(k).start()
    for copy in own[3:5]:
        copy.wait()
    for j in range(CUTS):
        tokens(1, j).start()
        gu(4, j).start()
        if j == 0:
            tokens(2).start()
            gu(1).start()
        if j % (CUTS // NEAR_CUTS) == 0:
            gu(2, j * NEAR_CUTS // CUTS).start()
    own[5].wait()
    dn(1).start()
    dn(2).start()
    for j in range(AHEAD):
        dn(4, j).start()
    own[7].wait()
    ranks(0)
    routes(1).wait_recv()
    routes(3).start()
    routes(2).wait_recv()
    gather(0)
    spread(0, 0, mine)
    ranks(1)
    ranks(2)
    spread(0, 2, of_x)

    def far(j):
        gu(4, j).wait_recv()
        gu(6, j).start()
        gu(5, j).start()

    def far_mate(j):
        gu(6, j).wait_recv()
        gu(7, j).start()

    def down_far(j):
        dn(4, j).wait_recv()
        if j + AHEAD < CUTS:
            dn(4, j + AHEAD).start()
        dn(6, j).start()
        dn(5, j).start()

    def down_mate(j):
        dn(6, j).wait_recv()
        dn(7, j).start()

    def near(j):
        SN[j, :cap] = down(0, 1, 1, j)
        first(0, j, pl.ds(0, cap)).start()

    x_first = [j for j in range(CUTS) if j not in Z_FIRST]
    for i in range(CUTS):
        tokens(1, i).wait_recv()
        tokens(3, i).start()
        far(i)
        if i < NEAR_CUTS:
            gu(2, i).wait_recv()
            gu(3, i).start()
        if i == 0:
            spread(0, 4, of_z)
            spread(1, 6, mine)
        if i == 1:
            spread(1, 8, of_x)
            spread(2, 10, mine)
        if i == 2:
            spread(2, 12, of_z)
        if i == NEAR_CUTS - 1:
            routes(3).wait_recv()
            ranks(3)
        if i == NEAR_CUTS:
            tokens(2).wait_recv()
            gather(2)
            gu(1).wait_recv()
            gu(3).wait_recv()
            hidden(0, 4, 0, 2)
        if i == NEAR_CUTS + 1:
            dn(2).wait_recv()
            dn(3).start()
            far_mate(0)
            dn(1).wait_recv()
            dn(3).wait_recv()
            near(x_first[0])
        if i == NEAR_CUTS + 2:
            far_mate(1)
            near(x_first[1])
            far_mate(2)
    gather(1)
    for j in x_first[2:]:
        near(j)
    far_mate(3)
    tokens(3).wait_recv()
    gather(3)
    far_mate(4)
    hidden(0, 4, 2, 4)
    for j in x_first:
        SN[j, cap:] = down(0, 2, 1, j)
        first(1, j, pl.ds(cap, cap)).start()
    far_mate(5)
    for j in Z_FIRST:
        SN[j] = down(0, 2, 2, j)
        first(1, j).start()
    down_far(0)
    far_mate(6)
    gu(5).wait_recv()
    hidden(4, 6, 0, 4)
    far_mate(7)
    down_far(1)
    down_far(2)
    widen(0, 0, (0,))
    down_mate(0)
    gu(7).wait_recv()
    hidden(6, 8, 0, 4)
    down_far(3)

    def pass_on(j):
        first(2, j).wait_recv()
        if j in Z_FIRST:
            first(1, j).wait_recv()
            kept, base, home, from_home, at = 2, 12, 4, 1, 0
        else:
            first(0, j, pl.ds(0, cap)).wait_recv()
            first(1, j, pl.ds(cap, cap)).wait_recv()
            kept, base, home, from_home, at = 1, 8, 2, 0, 1
        ZS[j] = total(kept, base, at, j).astype(bf)
        second(j).start()
        ACC[j] = total(0, home, from_home, j)

    for j in range(CUTS):
        if j + 1 < CUTS:
            down_mate(j + 1)
        dn(5, j).wait_recv()
        dn(7, j).wait_recv()
        SF[j] = down(1, 2 if j in Z_FIRST else 1, 2, j)
        first(2, j).start()
        if j + 4 < CUTS:
            down_far(j + 4)
        if j == 0:
            widen(1, 6, (0, 1))
            widen(2, 10, (0, 1))
            widen(0, 0, (1,))
        if j >= LAG:
            pass_on(j - LAG)
    for j in range(CUTS - LAG, CUTS):
        pass_on(j)
    square = jnp.zeros((count, 1), f32)
    for j in range(CUTS):
        second(j).wait_recv()
        mixed = ACC[j] + ZR[j].astype(f32)
        ACC[j] = mixed
        square = square + jnp.sum(mixed * mixed, axis=1, keepdims=True)
    scale = lax.rsqrt(square / width + 1e-06)
    for j in range(CUTS):
        out[:, lane_block(j)] = (ACC[j] * scale * POST[:, lane_block(j)]).astype(bf)
    for k in (1, 2, 3):
        routes(k).wait_send()
        tokens(k).wait_send()
    for k in range(1, 8):
        gu(k).wait_send()
        dn(k).wait_send()
    for kind, (src, dst) in enumerate(((SN, RN), (SF, RF), (ZS, ZR))):
        remote(src, dst, s_send.at[kind], z_recv.at[0], to_x).wait_send()


def fused(n_ep, tokens, pre_gain, post_gain, expert_ids, route_weight, w_gate, w_up, w_down):
    count, width = tokens.shape
    top = expert_ids.shape[1]
    part = w_gate.shape[2]
    experts = n_ep * w_gate.shape[0]
    cap = 2 * top * count // experts
    bf, f32 = jnp.bfloat16, jnp.float32
    cols = width // CUTS
    anywhere = pl.BlockSpec(memory_space=pl.ANY)
    vmem = pl.BlockSpec(memory_space=pltpu.VMEM)
    dma = pltpu.SemaphoreType.DMA
    return pl.pallas_call(
        functools.partial(kernel, n_ep),
        out_shape=jax.ShapeDtypeStruct((count, width), bf),
        in_specs=[anywhere] * 8,
        out_specs=vmem,
        scratch_shapes=[
            pltpu.VMEM((count, width), bf),
            pltpu.VMEM((4, count, width), bf),
            pltpu.VMEM((2, 4 * cap, width), bf),
            pltpu.VMEM((top, count), jnp.int32),
            pltpu.VMEM((top, count), f32),
            pltpu.VMEM((1, width), f32),
            pltpu.VMEM((1, width), f32),
            pltpu.VMEM((4, experts, count), f32),
            pltpu.VMEM((4, experts, count), f32),
            pltpu.VMEM((2, 4 * cap, part), f32),
            pltpu.VMEM((8, width, 2 * part), bf),
            pltpu.VMEM((width, 8 * part), bf),
            pltpu.VMEM((2, 4 * cap, 4 * part), bf),
            pltpu.VMEM((3, count, 8 * part), bf),
            pltpu.VMEM((14, count, cap), bf),
            pltpu.VMEM((CUTS, 2 * cap, cols), bf),
            pltpu.VMEM((CUTS, 2 * cap, cols), bf),
            pltpu.VMEM((CUTS, 2 * cap, cols), bf),
            pltpu.VMEM((CUTS, 2 * cap, cols), bf),
            pltpu.VMEM((CUTS, count, cols), bf),
            pltpu.VMEM((CUTS, count, cols), bf),
            pltpu.VMEM((CUTS, count, cols), f32),
            dma((8,)),
            dma((3,)), dma((CUTS,)), dma((3,)), dma((3,)), dma((3,)),
            dma((7,)), dma((7,)), dma((NEAR_CUTS,)), dma((2, CUTS)),
            dma((7,)), dma((3,)), dma((4, CUTS)),
            dma((3,)), dma((CUTS,)), dma((CUTS,)), dma((CUTS,)), dma((CUTS,)),
        ],
        compiler_params=pltpu.CompilerParams(
            collective_id=0, has_side_effects=True, vmem_limit_bytes=VMEM_BYTES
        ),
    )(tokens, pre_gain[None], post_gain[None], expert_ids.T, route_weight.T, w_gate, w_up, w_down)


def whole_body(n_ep, n_tp, *args):
    lanes = args[5].shape[2]
    if n_ep // 2 == n_tp == 2 * 2 and args[5].shape[0] == 1 and lanes % 128 == 0:
        return fused(n_ep, *args)
    return body(*args)


def solution(mesh):
    in_specs = (
        P(("ep", "tp"), None),
        P(),
        P(),
        P(("ep", "tp"), None),
        P(("ep", "tp"), None),
        P("ep", None, "tp"),
        P("ep", None, "tp"),
        P("ep", None, "tp"),
    )
    out_specs = P(("ep", "tp"), None)
    step = functools.partial(whole_body, mesh.shape["ep"], mesh.shape["tp"])
    return jax.shard_map(step, mesh=mesh, in_specs=in_specs, out_specs=out_specs, check_vma=False)
```

```python
import functools

import jax
import jax.numpy as jnp
from jax import lax
from jax.experimental import pallas as pl
from jax.experimental.pallas import tpu as pltpu
from jax.sharding import PartitionSpec as P


def rms_scale(values, gain):
    mean_sq = jnp.mean(values * values, axis=-1, keepdims=True)
    return values * lax.rsqrt(mean_sq + 1e-06) * gain


def expert_terms(rows, gate_part, up_part, down_part):
    gate = jnp.dot(rows, gate_part, preferred_element_type=jnp.float32)
    up = jnp.dot(rows, up_part, preferred_element_type=jnp.float32)
    hidden = (jax.nn.silu(gate) * up).astype(jnp.bfloat16)
    return lax.dot_general(
        hidden, down_part, (((1,), (1,)), ((), ())), preferred_element_type=jnp.float32
    )


def collect_expert(w_gate, w_up, w_down):
    return (
        lax.all_gather(w_gate, "tp", axis=2, tiled=True),
        lax.all_gather(w_up, "tp", axis=2, tiled=True),
        lax.all_gather(w_down, "tp", axis=2, tiled=True),
    )


def body(tokens, pre_gain, post_gain, expert_ids, route_weight, w_gate, w_up, w_down):
    count, width = tokens.shape
    top = expert_ids.shape[1]
    experts = lax.axis_size("ep") * w_gate.shape[0]
    capacity = 2 * top * count // experts
    normed = rms_scale(tokens.astype(jnp.float32), pre_gain).astype(jnp.bfloat16)
    flat = expert_ids.reshape(-1)
    onehot = (flat[:, None] == jnp.arange(experts, dtype=jnp.int32)[None, :]).astype(jnp.int32)
    rank = jnp.sum((jnp.cumsum(onehot, axis=0) - onehot) * onehot, axis=1)
    target = flat * capacity + rank
    source = jnp.full((experts * capacity,), count, jnp.int32)
    source = source.at[target].set(jnp.arange(count * top, dtype=jnp.int32) // top)
    padded = jnp.concatenate([normed, jnp.zeros((1, width), jnp.bfloat16)], axis=0)
    outgoing = padded[source].reshape(experts, capacity, width)
    arrived = lax.all_to_all(outgoing, "ep", split_axis=0, concat_axis=0, tiled=True)
    rows = arrived.reshape(experts * capacity, width)
    gate_all, up_all, down_all = collect_expert(w_gate, w_up, w_down)
    result = expert_terms(rows, gate_all[0], up_all[0], down_all[0])
    answer = result.astype(jnp.bfloat16).reshape(experts, capacity, width)
    returned = lax.all_to_all(answer, "ep", split_axis=0, concat_axis=0, tiled=True)
    per_route = returned.reshape(experts * capacity, width)[target].reshape(count, top, width)
    mixed = jnp.sum(per_route.astype(jnp.float32) * route_weight[:, :, None], axis=1)
    return rms_scale(mixed, post_gain).astype(jnp.bfloat16)

MESH = pl.DeviceIdType.MESH
CUTS = 8
NEAR_CUTS = 4
AHEAD = 4
Z_FIRST = (0,)
PLACE = (0, 3, 1, 2)
VMEM_BYTES = 60 * 2**20


def flip(index, stride):
    return index + stride - 2 * stride * lax.rem(lax.div(index, stride), 2)


def kernel(
    n_ep, tok, pre, post, ids, rw, wg, wu, wd, out,
    T, X, XC, IDS, RW, PRE, POST, WR, RK, COL, GU, DN, H, HX, EC, SN, SF, RN, RF, ZS, ZR, ACC,
    loc, t_send, t1_recv, t_recv, w_send, w_recv, g_send, g_recv, g2_recv, gf_recv, d_send, d_recv, df_recv,
    s_send, n_recv, m_recv, f_recv, h_recv, z_recv,
):
    count, width = tok.shape
    part = wg.shape[2]
    experts = WR.shape[1]
    cap = EC.shape[2]
    half = n_ep // 2
    bf, f32 = jnp.bfloat16, jnp.float32
    e, t = lax.axis_index("ep"), lax.axis_index("tp")
    to_x, to_z, to_h = (flip(e, 1), t), (flip(e, 2), t), (flip(e, half), t)
    to_c, to_y = (e, flip(t, 1)), (e, flip(t, 2))

    barrier = pltpu.get_barrier_semaphore()
    for who in (to_x, to_z, to_h, to_c, to_y):
        pl.semaphore_signal(barrier, inc=1, device_id=who, device_id_type=MESH)

    own = [
        pltpu.make_async_copy(ids, IDS, loc.at[0]),
        pltpu.make_async_copy(rw, RW, loc.at[1]),
        pltpu.make_async_copy(tok, T, loc.at[2]),
        pltpu.make_async_copy(wg.at[0], GU.at[0, :, pl.ds(0, part)], loc.at[3]),
        pltpu.make_async_copy(wu.at[0], GU.at[0, :, pl.ds(part, part)], loc.at[4]),
        pltpu.make_async_copy(wd.at[0], DN.at[:, pl.ds(0, part)], loc.at[5]),
        pltpu.make_async_copy(pre, PRE, loc.at[6]),
        pltpu.make_async_copy(post, POST, loc.at[7]),
    ]
    for copy in own:
        copy.start()

    def remote(src, dst, send, recv, who):
        return pltpu.make_async_remote_copy(
            src_ref=src, dst_ref=dst, send_sem=send, recv_sem=recv, device_id=who, device_id_type=MESH
        )

    def rows_of(total, cuts, j):
        return pl.ds(0, total) if j is None else pl.ds(j * (total // cuts), total // cuts)

    block_from = {1: (0, to_z), 2: (0, to_x), 3: (1, to_x)}

    def routes(k):
        s, who = block_from[k]
        return remote(WR.at[s], WR.at[k], w_send.at[k - 1], w_recv.at[k - 1], who)

    def tokens(k, j=None):
        s, who = block_from[k]
        rows = rows_of(count, CUTS, j)
        recv = t1_recv.at[j] if k == 1 and j is not None else t_recv.at[k - 1]
        return remote(X.at[s, rows], X.at[k, rows], t_send.at[k - 1], recv, who)

    def route(k):
        if k % 2:
            return k - 1, to_c
        if k % 4:
            return k - 2, to_y
        return 0, to_h

    def gu(k, j=None):
        s, who = route(k)
        rows = rows_of(width, NEAR_CUTS if k in (2, 3) else CUTS, j)
        recv = g_recv.at[k - 1]
        if j is not None and k == 2:
            recv = g2_recv.at[j]
        if j is not None and k in (4, 6):
            recv = gf_recv.at[k // 2 - 2, j]
        return remote(GU.at[s, rows], GU.at[k, rows], g_send.at[k - 1], recv, who)

    def dn(k, j=None):
        s, who = route(k)
        rows = rows_of(width, CUTS, j)
        recv = d_recv.at[k - 1] if k < 4 else df_recv.at[k - 4, 0 if j is None else j]
        return remote(
            DN.at[rows, pl.ds(s * part, part)], DN.at[rows, pl.ds(k * part, part)], d_send.at[k - 1], recv, who
        )

    cols = width // CUTS

    def lane_block(j):
        return pl.ds(j * cols, cols)

    def first(kind, j, rows=None):
        src, dst = (SN, RN) if kind < 2 else (SF, RF)
        rows = pl.ds(0, 2 * cap) if rows is None else rows
        recv = (n_recv, m_recv, f_recv, h_recv)[kind].at[j]
        return remote(src.at[j, rows], dst.at[j, rows], s_send.at[kind // 2], recv, to_z if j in Z_FIRST else to_x)

    def second(j):
        return remote(ZS.at[j], ZR.at[j], s_send.at[2], z_recv.at[j], to_x if j in Z_FIRST else to_z)

    which = lax.broadcasted_iota(jnp.int32, (experts, count), 0)
    mine = (e, lax.rem(e + half, n_ep))
    of_x = (flip(e, 1), lax.rem(flip(e, 1) + half, n_ep))
    of_z = (flip(e, 2), lax.rem(flip(e, 2) + half, n_ep))

    def row_of(table, expert):
        return jnp.sum(jnp.where(which == expert, table, 0.0), axis=0, keepdims=True)

    def own_routes():
        picks = [jnp.where(IDS[k : k + 1, :] == which, RW[k : k + 1, :], 0.0) for k in range(ids.shape[0])]
        total = picks[0]
        for pick in picks[1:]:
            total = total + pick
        WR[0] = total

    def ranks(block):
        named = WR[block] > 0.0
        ones = jnp.where(named, 1.0, 0.0)
        before = lax.broadcasted_iota(jnp.int32, (count, count), 0) <= lax.broadcasted_iota(
            jnp.int32, (count, count), 1
        )
        upto = jnp.dot(ones, jnp.where(before, 1.0, 0.0), preferred_element_type=f32)
        RK[block] = jnp.where(named, upto - 1.0, -1.0)

    def norm():
        def some(i, carry):
            rows = pl.ds(pl.multiple_of(i * 16, 16), 16)
            X[0, rows, :] = rms_scale(T[rows, :].astype(f32), PRE[...]).astype(bf)
            return carry

        lax.fori_loop(0, count // 16, some, 0, unroll=4)

    def gather(block):
        rows = pl.ds(PLACE[block] * cap, cap)
        picks = []
        for h in range(2):
            at = row_of(RK[block], mine[h])
            hit = lax.broadcasted_iota(jnp.int32, (cap, count), 0).astype(f32) == at
            weight = jnp.sum(jnp.where(hit, row_of(WR[block], mine[h]), 0.0), axis=1, keepdims=True)
            COL[h, rows, :] = jnp.broadcast_to(weight, (cap, part))
            picks.append(jnp.where(hit, 1.0, 0.0).astype(bf))
        pick = jnp.concatenate(picks, axis=0)
        step = width // 4
        for i in range(4):
            lanes = pl.ds(i * step, step)
            found = jnp.dot(pick, X[block, :, lanes], preferred_element_type=f32).astype(bf)
            XC[0, rows, lanes] = found[:cap]
            XC[1, rows, lanes] = found[cap:]

    def spread(block, base, whose):
        eye = lax.broadcasted_iota(jnp.int32, (count, count), 0) == lax.broadcasted_iota(
            jnp.int32, (count, count), 1
        )
        for h in range(2):
            at = jnp.sum(jnp.where(eye, row_of(RK[block], whose[h]), 0.0), axis=1, keepdims=True)
            hit = lax.broadcasted_iota(jnp.int32, (count, cap), 1).astype(f32) == at
            EC[base + h] = jnp.where(hit, 1.0, 0.0).astype(bf)

    def hidden(low, high, a, b):
        h = low // 4
        rows = pl.ds(a * cap, (b - a) * cap)

        def one(s, carry):
            both = jnp.dot(XC[h, rows, :], GU[s], preferred_element_type=f32)
            gate, up = both[:, :part], both[:, part:]
            value = gate / (1.0 + jnp.exp(-gate)) * up * COL[h, rows, :]
            H[h, rows, pl.ds(pl.multiple_of((s - 4 * h) * part, part), part)] = value.astype(bf)
            return carry

        lax.fori_loop(low, high, one, 0)

    def times(left, right):
        return lax.dot_general(left, right, (((1,), (1,)), ((), ())), preferred_element_type=f32)

    def down(h, place, n, j):
        left = H[h, pl.ds(place * cap, n * cap), :]
        return times(left, DN[lane_block(j), pl.ds(h * 4 * part, 4 * part)]).astype(bf)

    def widen(block, base, halves):
        for h in halves:
            left = jnp.dot(EC[base + h], H[h, pl.ds(PLACE[block] * cap, cap), :], preferred_element_type=f32)
            HX[block, :, pl.ds(h * 4 * part, 4 * part)] = left.astype(bf)

    def total(block, base, at, j):
        rows = pl.ds(at * cap, cap)
        return (
            times(HX[block], DN[lane_block(j), :])
            + jnp.dot(EC[base], RN[j, rows, :], preferred_element_type=f32)
            + jnp.dot(EC[base + 1], RF[j, rows, :], preferred_element_type=f32)
        )

    for copy in own[:2]:
        copy.wait()
    own_routes()
    own[2].wait()
    own[6].wait()
    norm()
    pl.semaphore_wait(barrier, 5)
    for k in (1, 2):
        routes(k).start()
    for copy in own[3:5]:
        copy.wait()
    for j in range(CUTS):
        tokens(1, j).start()
        gu(4, j).start()
        if j == 0:
            tokens(2).start()
            gu(1).start()
        if j % (CUTS // NEAR_CUTS) == 0:
            gu(2, j * NEAR_CUTS // CUTS).start()
    own[5].wait()
    dn(1).start()
    dn(2).start()
    for j in range(AHEAD):
        dn(4, j).start()
    own[7].wait()
    ranks(0)
    routes(1).wait_recv()
    routes(3).start()
    routes(2).wait_recv()
    gather(0)
    spread(0, 0, mine)
    ranks(1)
    ranks(2)
    spread(0, 2, of_x)

    def far(j):
        gu(4, j).wait_recv()
        gu(6, j).start()
        gu(5, j).start()

    def far_mate(j):
        gu(6, j).wait_recv()
        gu(7, j).start()

    def down_far(j):
        dn(4, j).wait_recv()
        if j + AHEAD < CUTS:
            dn(4, j + AHEAD).start()
        dn(6, j).start()
        dn(5, j).start()

    def down_mate(j):
        dn(6, j).wait_recv()
        dn(7, j).start()

    def near(j):
        SN[j, :cap] = down(0, 1, 1, j)
        first(0, j, pl.ds(0, cap)).start()

    def chunk(j):
        if j in Z_FIRST:
            return 2, 12, 4, 1, 0
        return 1, 8, 2, 0, 1

    def parts(j):
        near_rows, far_rows = pl.ds(0, cap), pl.ds(cap, cap)
        return (far_rows, near_rows) if j in Z_FIRST else (near_rows, far_rows)

    def relay(j):
        kept, base, _, _, at = chunk(j)
        first(2, j, parts(j)[1]).wait_recv()
        if j in Z_FIRST:
            first(1, j).wait_recv()
        else:
            first(0, j, pl.ds(0, cap)).wait_recv()
            first(1, j, pl.ds(cap, cap)).wait_recv()
        ZS[j] = total(kept, base, at, j).astype(bf)
        second(j).start()

    def settle(j):
        _, _, base, at, _ = chunk(j)
        first(3, j, parts(j)[0]).wait_recv()
        ACC[j] = total(0, base, at, j)

    x_first = [j for j in range(CUTS) if j not in Z_FIRST]

    def near(i):
        if i < len(x_first):
            SN[x_first[i], :cap] = down(0, 1, 1, x_first[i])
            first(0, x_first[i], pl.ds(0, cap)).start()

    def diagonal(j):
        if j in Z_FIRST:
            SN[j] = down(0, 2, 2, j)
            first(1, j).start()
        else:
            SN[j, cap:] = down(0, 2, 1, j)
            first(1, j, pl.ds(cap, cap)).start()

    def foreign(j):
        dn(5, j).wait_recv()
        dn(7, j).wait_recv()
        SF[j] = down(1, 2 if j in Z_FIRST else 1, 2, j)
        first(2, j, parts(j)[1]).start()

    def push(j):
        first(3, j, parts(j)[0]).start()

    def one_token(i):
        tokens(1, i).wait_recv()
        tokens(3, i).start()

    def near_mate(i):
        gu(2, i).wait_recv()
        gu(3, i).start()

    def block_two():
        tokens(2).wait_recv()
        gather(2)

    def native_early():
        gu(1).wait_recv()
        gu(3).wait_recv()
        hidden(0, 4, 0, 2)

    def down_two():
        dn(2).wait_recv()
        dn(3).start()

    def down_near():
        dn(1).wait_recv()
        dn(3).wait_recv()

    def block_three():
        tokens(3).wait_recv()
        gather(3)

    def far_low():
        gu(5).wait_recv()
        hidden(4, 6, 0, 4)

    def far_high():
        gu(7).wait_recv()
        hidden(6, 8, 0, 4)

    def routes_three():
        routes(3).wait_recv()
        ranks(3)

    def widen_all(h):
        widen(1, 6, (h,))
        widen(2, 10, (h,))
        widen(0, 0, (h,))

    one_token(0)
    far(0)
    near_mate(0)
    spread(0, 4, of_z)
    spread(1, 6, mine)
    one_token(1)
    far(1)
    near_mate(1)
    spread(1, 8, of_x)
    spread(2, 10, mine)
    one_token(2)
    far(2)
    near_mate(2)
    spread(2, 12, of_z)
    one_token(3)
    far(3)
    near_mate(3)
    routes_three()
    one_token(4)
    far(4)
    block_two()
    native_early()
    one_token(5)
    far(5)
    down_two()
    far_mate(0)
    down_near()
    near(0)
    one_token(6)
    far(6)
    far_mate(1)
    near(1)
    far_mate(2)
    one_token(7)
    far(7)
    gather(1)
    near(2)
    near(3)
    near(4)
    near(5)
    near(6)
    near(7)
    far_mate(3)
    block_three()
    far_mate(4)
    hidden(0, 4, 2, 4)
    diagonal(1)
    diagonal(2)
    diagonal(3)
    diagonal(4)
    diagonal(5)
    diagonal(6)
    diagonal(7)
    far_mate(5)
    diagonal(0)
    down_far(0)
    far_mate(6)
    far_low()
    far_mate(7)
    down_far(1)
    down_far(2)
    widen_all(0)
    down_mate(0)
    far_high()
    down_far(3)
    down_mate(1)
    foreign(0)
    down_mate(2)
    foreign(1)
    widen_all(1)
    down_far(4)
    down_mate(3)
    foreign(2)
    down_far(5)
    push(0)
    down_mate(4)
    foreign(3)
    down_far(6)
    push(1)
    relay(1)
    down_mate(5)
    foreign(4)
    down_far(7)
    push(2)
    relay(2)
    down_mate(6)
    foreign(5)
    push(3)
    relay(3)
    down_mate(7)
    foreign(6)
    push(4)
    relay(4)
    foreign(7)
    push(5)
    relay(5)
    push(6)
    push(7)
    relay(0)
    settle(0)
    settle(1)
    relay(6)
    settle(2)
    settle(3)
    relay(7)
    settle(4)
    settle(5)
    settle(6)
    settle(7)
    square = jnp.zeros((count, 1), f32)
    for j in (1, 2, 3, 4, 5, 0, 6, 7):
        second(j).wait_recv()
        mixed = ACC[j] + ZR[j].astype(f32)
        ACC[j] = mixed
        square = square + jnp.sum(mixed * mixed, axis=1, keepdims=True)
    scale = lax.rsqrt(square / width + 1e-06)
    for j in range(CUTS):
        out[:, lane_block(j)] = (ACC[j] * scale * POST[:, lane_block(j)]).astype(bf)
    for k in (1, 2, 3):
        routes(k).wait_send()
        tokens(k).wait_send()
    for k in range(1, 8):
        gu(k).wait_send()
        dn(k).wait_send()
    for kind, (src, dst) in enumerate(((SN, RN), (SF, RF), (ZS, ZR))):
        remote(src, dst, s_send.at[kind], z_recv.at[0], to_x).wait_send()


def fused(n_ep, tokens, pre_gain, post_gain, expert_ids, route_weight, w_gate, w_up, w_down):
    count, width = tokens.shape
    top = expert_ids.shape[1]
    part = w_gate.shape[2]
    experts = n_ep * w_gate.shape[0]
    cap = 2 * top * count // experts
    bf, f32 = jnp.bfloat16, jnp.float32
    cols = width // CUTS
    anywhere = pl.BlockSpec(memory_space=pl.ANY)
    vmem = pl.BlockSpec(memory_space=pltpu.VMEM)
    dma = pltpu.SemaphoreType.DMA
    return pl.pallas_call(
        functools.partial(kernel, n_ep),
        out_shape=jax.ShapeDtypeStruct((count, width), bf),
        in_specs=[anywhere] * 8,
        out_specs=vmem,
        scratch_shapes=[
            pltpu.VMEM((count, width), bf),
            pltpu.VMEM((4, count, width), bf),
            pltpu.VMEM((2, 4 * cap, width), bf),
            pltpu.VMEM((top, count), jnp.int32),
            pltpu.VMEM((top, count), f32),
            pltpu.VMEM((1, width), f32),
            pltpu.VMEM((1, width), f32),
            pltpu.VMEM((4, experts, count), f32),
            pltpu.VMEM((4, experts, count), f32),
            pltpu.VMEM((2, 4 * cap, part), f32),
            pltpu.VMEM((8, width, 2 * part), bf),
            pltpu.VMEM((width, 8 * part), bf),
            pltpu.VMEM((2, 4 * cap, 4 * part), bf),
            pltpu.VMEM((3, count, 8 * part), bf),
            pltpu.VMEM((14, count, cap), bf),
            pltpu.VMEM((CUTS, 2 * cap, cols), bf),
            pltpu.VMEM((CUTS, 2 * cap, cols), bf),
            pltpu.VMEM((CUTS, 2 * cap, cols), bf),
            pltpu.VMEM((CUTS, 2 * cap, cols), bf),
            pltpu.VMEM((CUTS, count, cols), bf),
            pltpu.VMEM((CUTS, count, cols), bf),
            pltpu.VMEM((CUTS, count, cols), f32),
            dma((8,)),
            dma((3,)), dma((CUTS,)), dma((3,)), dma((3,)), dma((3,)),
            dma((7,)), dma((7,)), dma((NEAR_CUTS,)), dma((2, CUTS)),
            dma((7,)), dma((3,)), dma((4, CUTS)),
            dma((3,)), dma((CUTS,)), dma((CUTS,)), dma((CUTS,)), dma((CUTS,)), dma((CUTS,)),
        ],
        compiler_params=pltpu.CompilerParams(
            collective_id=0, has_side_effects=True, vmem_limit_bytes=VMEM_BYTES
        ),
    )(tokens, pre_gain[None], post_gain[None], expert_ids.T, route_weight.T, w_gate, w_up, w_down)


def whole_body(n_ep, n_tp, *args):
    lanes = args[5].shape[2]
    if n_ep // 2 == n_tp == 2 * 2 and args[5].shape[0] == 1 and lanes % 128 == 0:
        return fused(n_ep, *args)
    return body(*args)


def solution(mesh):
    in_specs = (
        P(("ep", "tp"), None),
        P(),
        P(),
        P(("ep", "tp"), None),
        P(("ep", "tp"), None),
        P("ep", None, "tp"),
        P("ep", None, "tp"),
        P("ep", None, "tp"),
    )
    out_specs = P(("ep", "tp"), None)
    step = functools.partial(whole_body, mesh.shape["ep"], mesh.shape["tp"])
    return jax.shard_map(step, mesh=mesh, in_specs=in_specs, out_specs=out_specs, check_vma=False)
```

```python
import functools

import jax
import jax.numpy as jnp
from jax import lax
from jax.experimental import pallas as pl
from jax.experimental.pallas import tpu as pltpu
from jax.sharding import PartitionSpec as P


def rms_scale(values, gain):
    mean_sq = jnp.mean(values * values, axis=-1, keepdims=True)
    return values * lax.rsqrt(mean_sq + 1e-06) * gain


def expert_terms(rows, gate_part, up_part, down_part):
    gate = jnp.dot(rows, gate_part, preferred_element_type=jnp.float32)
    up = jnp.dot(rows, up_part, preferred_element_type=jnp.float32)
    hidden = (jax.nn.silu(gate) * up).astype(jnp.bfloat16)
    return lax.dot_general(
        hidden, down_part, (((1,), (1,)), ((), ())), preferred_element_type=jnp.float32
    )


def collect_expert(w_gate, w_up, w_down):
    return (
        lax.all_gather(w_gate, "tp", axis=2, tiled=True),
        lax.all_gather(w_up, "tp", axis=2, tiled=True),
        lax.all_gather(w_down, "tp", axis=2, tiled=True),
    )


def body(tokens, pre_gain, post_gain, expert_ids, route_weight, w_gate, w_up, w_down):
    count, width = tokens.shape
    top = expert_ids.shape[1]
    experts = lax.axis_size("ep") * w_gate.shape[0]
    capacity = 2 * top * count // experts
    normed = rms_scale(tokens.astype(jnp.float32), pre_gain).astype(jnp.bfloat16)
    flat = expert_ids.reshape(-1)
    onehot = (flat[:, None] == jnp.arange(experts, dtype=jnp.int32)[None, :]).astype(jnp.int32)
    rank = jnp.sum((jnp.cumsum(onehot, axis=0) - onehot) * onehot, axis=1)
    target = flat * capacity + rank
    source = jnp.full((experts * capacity,), count, jnp.int32)
    source = source.at[target].set(jnp.arange(count * top, dtype=jnp.int32) // top)
    padded = jnp.concatenate([normed, jnp.zeros((1, width), jnp.bfloat16)], axis=0)
    outgoing = padded[source].reshape(experts, capacity, width)
    arrived = lax.all_to_all(outgoing, "ep", split_axis=0, concat_axis=0, tiled=True)
    rows = arrived.reshape(experts * capacity, width)
    gate_all, up_all, down_all = collect_expert(w_gate, w_up, w_down)
    result = expert_terms(rows, gate_all[0], up_all[0], down_all[0])
    answer = result.astype(jnp.bfloat16).reshape(experts, capacity, width)
    returned = lax.all_to_all(answer, "ep", split_axis=0, concat_axis=0, tiled=True)
    per_route = returned.reshape(experts * capacity, width)[target].reshape(count, top, width)
    mixed = jnp.sum(per_route.astype(jnp.float32) * route_weight[:, :, None], axis=1)
    return rms_scale(mixed, post_gain).astype(jnp.bfloat16)

MESH = pl.DeviceIdType.MESH
CUTS = 8
NEAR_CUTS = 4
AHEAD = 4
Z_FIRST = (0,)
PLACE = (0, 3, 1, 2)
VMEM_BYTES = 60 * 2**20


def flip(index, stride):
    return index + stride - 2 * stride * lax.rem(lax.div(index, stride), 2)


def kernel(
    n_ep, tok, pre, post, ids, rw, wg, wu, wd, out,
    T, X, XC, IDS, RW, PRE, POST, WR, RK, COL, GU, DN, H, HX, EC, SN, SF, RN, RF, ZS, ZR, ACC,
    loc, t_send, t1_recv, t_recv, w_send, w_recv, g_send, g_recv, g2_recv, gf_recv, d_send, d_recv, df_recv,
    s_send, n_recv, m_recv, f_recv, h_recv, z_recv,
):
    count, width = tok.shape
    part = wg.shape[2]
    experts = WR.shape[1]
    cap = EC.shape[2]
    half = n_ep // 2
    bf, f32 = jnp.bfloat16, jnp.float32
    e, t = lax.axis_index("ep"), lax.axis_index("tp")
    to_x, to_z, to_h = (flip(e, 1), t), (flip(e, 2), t), (flip(e, half), t)
    to_c, to_y = (e, flip(t, 1)), (e, flip(t, 2))

    barrier = pltpu.get_barrier_semaphore()
    for who in (to_x, to_z, to_h, to_c, to_y):
        pl.semaphore_signal(barrier, inc=1, device_id=who, device_id_type=MESH)

    own = [
        pltpu.make_async_copy(ids, IDS, loc.at[0]),
        pltpu.make_async_copy(rw, RW, loc.at[1]),
        pltpu.make_async_copy(tok, T, loc.at[2]),
        pltpu.make_async_copy(wg.at[0], GU.at[0, :, pl.ds(0, part)], loc.at[3]),
        pltpu.make_async_copy(wu.at[0], GU.at[0, :, pl.ds(part, part)], loc.at[4]),
        pltpu.make_async_copy(wd.at[0], DN.at[:, pl.ds(0, part)], loc.at[5]),
        pltpu.make_async_copy(pre, PRE, loc.at[6]),
        pltpu.make_async_copy(post, POST, loc.at[7]),
    ]
    for copy in own:
        copy.start()

    def remote(src, dst, send, recv, who):
        return pltpu.make_async_remote_copy(
            src_ref=src, dst_ref=dst, send_sem=send, recv_sem=recv, device_id=who, device_id_type=MESH
        )

    def rows_of(total, cuts, j):
        return pl.ds(0, total) if j is None else pl.ds(j * (total // cuts), total // cuts)

    block_from = {1: (0, to_z), 2: (0, to_x), 3: (1, to_x)}

    def routes(k):
        s, who = block_from[k]
        return remote(WR.at[s], WR.at[k], w_send.at[k - 1], w_recv.at[k - 1], who)

    def tokens(k, j=None):
        s, who = block_from[k]
        rows = rows_of(count, CUTS, j)
        recv = t1_recv.at[j] if k == 1 and j is not None else t_recv.at[k - 1]
        return remote(X.at[s, rows], X.at[k, rows], t_send.at[k - 1], recv, who)

    def route(k):
        if k % 2:
            return k - 1, to_c
        if k % 4:
            return k - 2, to_y
        return 0, to_h

    def gu(k, j=None):
        s, who = route(k)
        rows = rows_of(width, NEAR_CUTS if k in (2, 3) else CUTS, j)
        recv = g_recv.at[k - 1]
        if j is not None and k == 2:
            recv = g2_recv.at[j]
        if j is not None and k in (4, 6):
            recv = gf_recv.at[k // 2 - 2, j]
        return remote(GU.at[s, rows], GU.at[k, rows], g_send.at[k - 1], recv, who)

    def dn(k, j=None):
        s, who = route(k)
        rows = rows_of(width, CUTS, j)
        recv = d_recv.at[k - 1] if k < 4 else df_recv.at[k - 4, 0 if j is None else j]
        return remote(
            DN.at[rows, pl.ds(s * part, part)], DN.at[rows, pl.ds(k * part, part)], d_send.at[k - 1], recv, who
        )

    cols = width // CUTS

    def lane_block(j):
        return pl.ds(j * cols, cols)

    def first(kind, j, rows=None):
        src, dst = (SN, RN) if kind < 2 else (SF, RF)
        rows = pl.ds(0, 2 * cap) if rows is None else rows
        recv = (n_recv, m_recv, f_recv, h_recv)[kind].at[j]
        return remote(src.at[j, rows], dst.at[j, rows], s_send.at[kind // 2], recv, to_z if j in Z_FIRST else to_x)

    def second(j):
        return remote(ZS.at[j], ZR.at[j], s_send.at[2], z_recv.at[j], to_x if j in Z_FIRST else to_z)

    which = lax.broadcasted_iota(jnp.int32, (experts, count), 0)
    mine = (e, lax.rem(e + half, n_ep))
    of_x = (flip(e, 1), lax.rem(flip(e, 1) + half, n_ep))
    of_z = (flip(e, 2), lax.rem(flip(e, 2) + half, n_ep))

    def row_of(table, expert):
        return jnp.sum(jnp.where(which == expert, table, 0.0), axis=0, keepdims=True)

    def own_routes():
        picks = [jnp.where(IDS[k : k + 1, :] == which, RW[k : k + 1, :], 0.0) for k in range(ids.shape[0])]
        total = picks[0]
        for pick in picks[1:]:
            total = total + pick
        WR[0] = total

    def ranks(block):
        named = WR[block] > 0.0
        ones = jnp.where(named, 1.0, 0.0)
        before = lax.broadcasted_iota(jnp.int32, (count, count), 0) <= lax.broadcasted_iota(
            jnp.int32, (count, count), 1
        )
        upto = jnp.dot(ones, jnp.where(before, 1.0, 0.0), preferred_element_type=f32)
        RK[block] = jnp.where(named, upto - 1.0, -1.0)

    def norm():
        def some(i, carry):
            rows = pl.ds(pl.multiple_of(i * 16, 16), 16)
            X[0, rows, :] = rms_scale(T[rows, :].astype(f32), PRE[...]).astype(bf)
            return carry

        lax.fori_loop(0, count // 16, some, 0, unroll=4)

    def gather(block):
        rows = pl.ds(PLACE[block] * cap, cap)
        picks = []
        for h in range(2):
            at = row_of(RK[block], mine[h])
            hit = lax.broadcasted_iota(jnp.int32, (cap, count), 0).astype(f32) == at
            weight = jnp.sum(jnp.where(hit, row_of(WR[block], mine[h]), 0.0), axis=1, keepdims=True)
            COL[h, rows, :] = jnp.broadcast_to(weight, (cap, part))
            picks.append(jnp.where(hit, 1.0, 0.0).astype(bf))
        pick = jnp.concatenate(picks, axis=0)
        step = width // 4
        for i in range(4):
            lanes = pl.ds(i * step, step)
            found = jnp.dot(pick, X[block, :, lanes], preferred_element_type=f32).astype(bf)
            XC[0, rows, lanes] = found[:cap]
            XC[1, rows, lanes] = found[cap:]

    def spread(block, base, whose):
        eye = lax.broadcasted_iota(jnp.int32, (count, count), 0) == lax.broadcasted_iota(
            jnp.int32, (count, count), 1
        )
        for h in range(2):
            at = jnp.sum(jnp.where(eye, row_of(RK[block], whose[h]), 0.0), axis=1, keepdims=True)
            hit = lax.broadcasted_iota(jnp.int32, (count, cap), 1).astype(f32) == at
            EC[base + h] = jnp.where(hit, 1.0, 0.0).astype(bf)

    def hidden(low, high, a, b):
        h = low // 4
        rows = pl.ds(a * cap, (b - a) * cap)

        def one(s, carry):
            both = jnp.dot(XC[h, rows, :], GU[s], preferred_element_type=f32)
            gate, up = both[:, :part], both[:, part:]
            value = gate / (1.0 + jnp.exp(-gate)) * up * COL[h, rows, :]
            H[h, rows, pl.ds(pl.multiple_of((s - 4 * h) * part, part), part)] = value.astype(bf)
            return carry

        lax.fori_loop(low, high, one, 0)

    def times(left, right):
        return lax.dot_general(left, right, (((1,), (1,)), ((), ())), preferred_element_type=f32)

    def down(h, place, n, j):
        left = H[h, pl.ds(place * cap, n * cap), :]
        return times(left, DN[lane_block(j), pl.ds(h * 4 * part, 4 * part)]).astype(bf)

    def widen(block, base, halves):
        for h in halves:
            left = jnp.dot(EC[base + h], H[h, pl.ds(PLACE[block] * cap, cap), :], preferred_element_type=f32)
            HX[block, :, pl.ds(h * 4 * part, 4 * part)] = left.astype(bf)

    def total(block, base, at, j):
        rows = pl.ds(at * cap, cap)
        return (
            times(HX[block], DN[lane_block(j), :])
            + jnp.dot(EC[base], RN[j, rows, :], preferred_element_type=f32)
            + jnp.dot(EC[base + 1], RF[j, rows, :], preferred_element_type=f32)
        )

    for copy in own[:2]:
        copy.wait()
    own_routes()
    own[2].wait()
    own[6].wait()
    norm()
    pl.semaphore_wait(barrier, 5)
    for k in (1, 2):
        routes(k).start()
    for copy in own[3:5]:
        copy.wait()
    for j in range(CUTS):
        tokens(1, j).start()
        gu(4, j).start()
        if j == 0:
            tokens(2).start()
            gu(1).start()
        if j % (CUTS // NEAR_CUTS) == 0:
            gu(2, j * NEAR_CUTS // CUTS).start()
    own[5].wait()
    dn(1).start()
    dn(2).start()
    for j in range(AHEAD):
        dn(4, j).start()
    own[7].wait()
    ranks(0)
    routes(1).wait_recv()
    routes(3).start()
    routes(2).wait_recv()
    gather(0)
    spread(0, 0, mine)
    ranks(1)
    ranks(2)
    spread(0, 2, of_x)

    def far(j):
        gu(4, j).wait_recv()
        gu(6, j).start()
        gu(5, j).start()

    def far_mate(j):
        gu(6, j).wait_recv()
        gu(7, j).start()

    def down_far(j):
        dn(4, j).wait_recv()
        if j + AHEAD < CUTS:
            dn(4, j + AHEAD).start()
        dn(6, j).start()
        dn(5, j).start()

    def down_mate(j):
        dn(6, j).wait_recv()
        dn(7, j).start()

    def near(j):
        SN[j, :cap] = down(0, 1, 1, j)
        first(0, j, pl.ds(0, cap)).start()

    def chunk(j):
        if j in Z_FIRST:
            return 2, 12, 4, 1, 0
        return 1, 8, 2, 0, 1

    def parts(j):
        near_rows, far_rows = pl.ds(0, cap), pl.ds(cap, cap)
        return (far_rows, near_rows) if j in Z_FIRST else (near_rows, far_rows)

    def relay(j):
        kept, base, _, _, at = chunk(j)
        first(2, j, parts(j)[1]).wait_recv()
        if j in Z_FIRST:
            first(1, j).wait_recv()
        else:
            first(0, j, pl.ds(0, cap)).wait_recv()
            first(1, j, pl.ds(cap, cap)).wait_recv()
        ZS[j] = total(kept, base, at, j).astype(bf)
        second(j).start()

    def settle(j):
        _, _, base, at, _ = chunk(j)
        first(3, j, parts(j)[0]).wait_recv()
        ACC[j] = total(0, base, at, j)

    x_first = [j for j in range(CUTS) if j not in Z_FIRST]

    def near(i):
        if i < len(x_first):
            SN[x_first[i], :cap] = down(0, 1, 1, x_first[i])
            first(0, x_first[i], pl.ds(0, cap)).start()

    def diagonal(j):
        if j in Z_FIRST:
            SN[j] = down(0, 2, 2, j)
            first(1, j).start()
        else:
            SN[j, cap:] = down(0, 2, 1, j)
            first(1, j, pl.ds(cap, cap)).start()

    def foreign(j):
        dn(5, j).wait_recv()
        dn(7, j).wait_recv()
        SF[j] = down(1, 2 if j in Z_FIRST else 1, 2, j)
        first(2, j, parts(j)[1]).start()

    def push(j):
        first(3, j, parts(j)[0]).start()

    def one_token(i):
        tokens(1, i).wait_recv()
        tokens(3, i).start()

    def near_mate(i):
        gu(2, i).wait_recv()
        gu(3, i).start()

    def block_two():
        tokens(2).wait_recv()
        gather(2)

    def native_early():
        gu(1).wait_recv()
        gu(3).wait_recv()
        hidden(0, 4, 0, 2)

    def down_two():
        dn(2).wait_recv()
        dn(3).start()

    def down_near():
        dn(1).wait_recv()
        dn(3).wait_recv()

    def block_three():
        tokens(3).wait_recv()
        gather(3)

    def far_low():
        gu(5).wait_recv()
        hidden(4, 6, 0, 4)

    def far_mid():
        hidden(6, 7, 0, 4)

    def far_high():
        gu(7).wait_recv()
        hidden(7, 8, 0, 4)

    def routes_three():
        routes(3).wait_recv()
        ranks(3)

    def widen_all(h):
        widen(1, 6, (h,))
        widen(2, 10, (h,))
        widen(0, 0, (h,))

    one_token(0)
    far(0)
    near_mate(0)
    spread(0, 4, of_z)
    spread(1, 6, mine)
    one_token(1)
    far(1)
    near_mate(1)
    spread(1, 8, of_x)
    spread(2, 10, mine)
    one_token(2)
    far(2)
    near_mate(2)
    spread(2, 12, of_z)
    one_token(3)
    far(3)
    near_mate(3)
    routes_three()
    one_token(4)
    far(4)
    block_two()
    native_early()
    one_token(5)
    far(5)
    down_two()
    far_mate(0)
    down_near()
    near(0)
    one_token(6)
    far(6)
    far_mate(1)
    near(1)
    far_mate(2)
    one_token(7)
    far(7)
    gather(1)
    near(2)
    near(3)
    near(4)
    near(5)
    near(6)
    near(7)
    far_mate(3)
    block_three()
    far_mate(4)
    hidden(0, 4, 2, 4)
    diagonal(1)
    diagonal(2)
    diagonal(3)
    diagonal(4)
    diagonal(5)
    diagonal(6)
    diagonal(7)
    far_mate(5)
    down_far(0)
    far_mate(6)
    diagonal(0)
    far_low()
    far_mate(7)
    down_far(1)
    down_far(2)
    widen_all(0)
    far_mid()
    down_mate(0)
    far_high()
    down_far(3)
    down_mate(1)
    foreign(0)
    down_mate(2)
    foreign(1)
    widen_all(1)
    down_far(4)
    down_mate(3)
    foreign(2)
    down_far(5)
    down_mate(4)
    foreign(3)
    down_far(6)
    push(0)
    relay(1)
    down_mate(5)
    foreign(4)
    down_far(7)
    push(1)
    relay(2)
    down_mate(6)
    foreign(5)
    push(2)
    relay(3)
    down_mate(7)
    foreign(6)
    push(3)
    relay(4)
    foreign(7)
    push(4)
    relay(5)
    push(5)
    push(6)
    push(7)
    relay(0)
    settle(0)
    settle(1)
    relay(6)
    settle(2)
    settle(3)
    relay(7)
    settle(4)
    settle(5)
    settle(6)
    settle(7)
    square = jnp.zeros((count, 1), f32)
    for j in (1, 2, 3, 4, 5, 0, 6, 7):
        second(j).wait_recv()
        mixed = ACC[j] + ZR[j].astype(f32)
        ACC[j] = mixed
        square = square + jnp.sum(mixed * mixed, axis=1, keepdims=True)
    scale = lax.rsqrt(square / width + 1e-06)
    for j in range(CUTS):
        out[:, lane_block(j)] = (ACC[j] * scale * POST[:, lane_block(j)]).astype(bf)
    for k in (1, 2, 3):
        routes(k).wait_send()
        tokens(k).wait_send()
    for k in range(1, 8):
        gu(k).wait_send()
        dn(k).wait_send()
    for kind, (src, dst) in enumerate(((SN, RN), (SF, RF), (ZS, ZR))):
        remote(src, dst, s_send.at[kind], z_recv.at[0], to_x).wait_send()


def fused(n_ep, tokens, pre_gain, post_gain, expert_ids, route_weight, w_gate, w_up, w_down):
    count, width = tokens.shape
    top = expert_ids.shape[1]
    part = w_gate.shape[2]
    experts = n_ep * w_gate.shape[0]
    cap = 2 * top * count // experts
    bf, f32 = jnp.bfloat16, jnp.float32
    cols = width // CUTS
    anywhere = pl.BlockSpec(memory_space=pl.ANY)
    vmem = pl.BlockSpec(memory_space=pltpu.VMEM)
    dma = pltpu.SemaphoreType.DMA
    return pl.pallas_call(
        functools.partial(kernel, n_ep),
        out_shape=jax.ShapeDtypeStruct((count, width), bf),
        in_specs=[anywhere] * 8,
        out_specs=vmem,
        scratch_shapes=[
            pltpu.VMEM((count, width), bf),
            pltpu.VMEM((4, count, width), bf),
            pltpu.VMEM((2, 4 * cap, width), bf),
            pltpu.VMEM((top, count), jnp.int32),
            pltpu.VMEM((top, count), f32),
            pltpu.VMEM((1, width), f32),
            pltpu.VMEM((1, width), f32),
            pltpu.VMEM((4, experts, count), f32),
            pltpu.VMEM((4, experts, count), f32),
            pltpu.VMEM((2, 4 * cap, part), f32),
            pltpu.VMEM((8, width, 2 * part), bf),
            pltpu.VMEM((width, 8 * part), bf),
            pltpu.VMEM((2, 4 * cap, 4 * part), bf),
            pltpu.VMEM((3, count, 8 * part), bf),
            pltpu.VMEM((14, count, cap), bf),
            pltpu.VMEM((CUTS, 2 * cap, cols), bf),
            pltpu.VMEM((CUTS, 2 * cap, cols), bf),
            pltpu.VMEM((CUTS, 2 * cap, cols), bf),
            pltpu.VMEM((CUTS, 2 * cap, cols), bf),
            pltpu.VMEM((CUTS, count, cols), bf),
            pltpu.VMEM((CUTS, count, cols), bf),
            pltpu.VMEM((CUTS, count, cols), f32),
            dma((8,)),
            dma((3,)), dma((CUTS,)), dma((3,)), dma((3,)), dma((3,)),
            dma((7,)), dma((7,)), dma((NEAR_CUTS,)), dma((2, CUTS)),
            dma((7,)), dma((3,)), dma((4, CUTS)),
            dma((3,)), dma((CUTS,)), dma((CUTS,)), dma((CUTS,)), dma((CUTS,)), dma((CUTS,)),
        ],
        compiler_params=pltpu.CompilerParams(
            collective_id=0, has_side_effects=True, vmem_limit_bytes=VMEM_BYTES
        ),
    )(tokens, pre_gain[None], post_gain[None], expert_ids.T, route_weight.T, w_gate, w_up, w_down)


def whole_body(n_ep, n_tp, *args):
    lanes = args[5].shape[2]
    if n_ep // 2 == n_tp == 2 * 2 and args[5].shape[0] == 1 and lanes % 128 == 0:
        return fused(n_ep, *args)
    return body(*args)


def solution(mesh):
    in_specs = (
        P(("ep", "tp"), None),
        P(),
        P(),
        P(("ep", "tp"), None),
        P(("ep", "tp"), None),
        P("ep", None, "tp"),
        P("ep", None, "tp"),
        P("ep", None, "tp"),
    )
    out_specs = P(("ep", "tp"), None)
    step = functools.partial(whole_body, mesh.shape["ep"], mesh.shape["tp"])
    return jax.shard_map(step, mesh=mesh, in_specs=in_specs, out_specs=out_specs, check_vma=False)
```
